32 devices in a mesh: sp: 4 (over y, x), dp: 8 (over z, core).
Axes of the slice: x: 2, y: 2, z: 4, core: 2. Of those that a mesh axis runs over, the one named last changes fastest.
Arguments:
- tokens: bfloat16 [8, 640, 2048], P('dp', 'sp'), may hold values from -42 to 42
- query_weight: bfloat16 [2048, 1024], P('dp'), may hold values from -1 to 1
- key_weight: bfloat16 [2048, 1024], P('dp'), may hold values from -1 to 1
- values: bfloat16 [8, 640, 1024], P('dp', 'sp'), may hold values from -6 to 6
- lambdas: float32 [16], replicated, may hold values from 0.3 to 0.8
- out_grad: bfloat16 [8, 640, 1024], P('dp', 'sp'), may hold values from -6 to 6
Outputs:
- tokens_grad: bfloat16 [8, 640, 2048], P('dp', 'sp')
- values_grad: bfloat16 [8, 640, 1024], P('dp', 'sp')
- query_weight_grad: float32 [2048, 1024], P('dp')
- key_weight_grad: float32 [2048, 1024], P('dp')
The draws below stay inside these ranges and needn't reach their ends.
All inputs are finite; a program needn't handle non-finite values.
Results may differ from the reference program's by a relative error of at most 0.029.
The reference program's roundings to bfloat16 on the way count: a program that leaves them out, or rounds other values in their place, can miss the bound.
Values may be sent and summed in bfloat16 or wider, within the bound.
A program may use at most 128 MiB of HBM per device.

```python
import math
import jax
import jax.numpy as jnp
from jax import lax

D = 2048
HEADS = 16
DQK = 32
SEQLEN = 640
BATCH = 8
QCOLS = 1024
VCOLS = 1024


def weight_normals(key):
    first_draw = jax.random.normal(jax.random.fold_in(key, 11), (D, QCOLS), jnp.float32)
    second_draw = jax.random.normal(jax.random.fold_in(key, 12), (D, QCOLS), jnp.float32)
    return (first_draw, second_draw)


def draw_query_weight(key, part):
    first_draw, second_draw = weight_normals(key)
    return (jnp.clip(first_draw, -6.0, 6.0) * math.sqrt(3.0 / D)).astype(jnp.bfloat16)


def draw_key_weight(key, part):
    first_draw, second_draw = weight_normals(key)
    blended = second_draw
    return (jnp.clip(blended, -6.0, 6.0) * math.sqrt(1.0 / D)).astype(jnp.bfloat16)


def draw_tokens(key, part):
    base_draw = jnp.clip(jax.random.normal(jax.random.fold_in(key, 21), (BATCH, SEQLEN, D), jnp.float32), -6.0, 6.0)
    return base_draw.astype(jnp.bfloat16)


def levels(rng, dims, split, smallest, largest):
    factor_of, own = 1.0, jax.random.fold_in(rng, 6)
    for dim, shards_of in split:
        draws = jnp.exp(jax.random.uniform(jax.random.fold_in(own, dim), (shards_of,), jnp.float32, smallest / len(split), largest / len(split)))
        factor_of = factor_of * jnp.repeat(draws, dims[dim] // shards_of).reshape([-1 if axis == dim else 1 for axis in range(len(dims))])
    return factor_of


def gaussian(own_key, shape, scale, reach, pieces=(), kind=jnp.bfloat16):
    level = levels(own_key, shape, pieces, -0.22, 0.18) if pieces else 1.0
    entries = jax.random.normal(own_key, shape, jnp.float32) * scale * level
    return jnp.minimum(jnp.maximum(entries, -reach), reach).astype(kind)


def setup_inputs(seed: int = 0) -> dict:
    arg_keys = jax.random.split(jax.random.key(seed), 7)
    tokens = draw_tokens(jax.random.fold_in(arg_keys[6], 71), 0)
    query_weight = draw_query_weight(jax.random.fold_in(arg_keys[6], 71), 0)
    key_weight = draw_key_weight(jax.random.fold_in(arg_keys[6], 71), 0)
    values = gaussian(arg_keys[3], (BATCH, SEQLEN, VCOLS), 1.0, 6.0, ((0, 8), (1, 4)))
    lambdas = jnp.clip(jax.random.uniform(arg_keys[4], (HEADS,), jnp.float32, 0.3, 0.8), 0.3, 0.8)
    out_grad = gaussian(arg_keys[5], (BATCH, SEQLEN, VCOLS), 1.0, 6.0, ((0, 8), (1, 4)))
    return dict(tokens=tokens, query_weight=query_weight, key_weight=key_weight, values=values, lambdas=lambdas, out_grad=out_grad)


NORM_EPS = 0.1
THETA = 10000.0

def rotation_tables(positions, vec_width):
    half_width = vec_width // 2
    freqs = jnp.exp(-math.log(THETA) * jnp.arange(half_width, dtype=jnp.float32) / half_width)
    angles = positions.astype(jnp.float32)[:, None] * freqs[None, :]
    return (jnp.cos(angles), jnp.sin(angles))

def rotate(field, cosine, sine_table, vec_width, sign_value):
    full_shape = field.shape
    grouped = field.reshape(full_shape[:-1] + (full_shape[-1] // vec_width, 2, vec_width // 2))
    first_half = grouped[..., 0, :]
    second_half = grouped[..., 1, :]
    cos_cols = cosine[:, None, :]
    sin_cols = sign_value * sine_table[:, None, :]
    turned = jnp.stack([first_half * cos_cols - second_half * sin_cols, second_half * cos_cols + first_half * sin_cols], axis=-2)
    return turned.reshape(full_shape)

def pair_product(pattern, first_op, second_op):
    return jnp.einsum(pattern, first_op.astype(jnp.float32), second_op.astype(jnp.float32))

def head_backward(query_rot, key_rot, value_rows, grad_rows, lambda_here, cosine, sine_table):
    seq_length = query_rot.shape[0]
    head_count = lambda_here.shape[0]
    qk_width = query_rot.shape[1] // (2 * head_count)
    value_width = value_rows.shape[1] // head_count
    block_rows = math.gcd(seq_length, 512)
    block_count = seq_length // block_rows
    inv_root = 1.0 / math.sqrt(qk_width)
    query_split = query_rot.reshape(block_count, block_rows, head_count, 2, qk_width)
    key_split = key_rot.reshape(seq_length, head_count, 2, qk_width)
    value_split = value_rows.reshape(seq_length, head_count, value_width)
    grad_split = grad_rows.reshape(block_count, block_rows, head_count, value_width)
    lambda_col = lambda_here[:, None, None]
    key_positions = jnp.arange(seq_length, dtype=jnp.int32)

    def block_step(carried, inputs):
        key_sum, value_sum = carried
        query_part, grad_part, block_start = inputs
        scores = pair_product('qhmd,khmd->hmqk', query_part, key_split) * inv_root
        query_positions = block_start + jnp.arange(block_rows, dtype=jnp.int32)
        causal_mask = key_positions[None, :] <= query_positions[:, None]
        scores = jnp.where(causal_mask, scores, -jnp.inf)
        row_max = lax.optimization_barrier(jnp.max(scores, axis=-1, keepdims=True))
        exp_scores = jnp.exp(scores - row_max)
        prob_maps = exp_scores / lax.optimization_barrier(jnp.sum(exp_scores, axis=-1, keepdims=True))
        weights = (prob_maps[:, 0] - lambda_col * prob_maps[:, 1]).astype(jnp.bfloat16)
        mixed_out = pair_product('hqk,khe->qhe', weights, value_split)
        norm_scale = lax.rsqrt(lax.optimization_barrier(jnp.mean(mixed_out * mixed_out, axis=-1, keepdims=True)) + NORM_EPS)
        grad_float = grad_part.astype(jnp.float32)
        mixed_grad = (norm_scale * grad_float - norm_scale * norm_scale * norm_scale * mixed_out * lax.optimization_barrier(jnp.mean(grad_float * mixed_out, axis=-1, keepdims=True))).astype(jnp.bfloat16)
        weight_grad = pair_product('qhe,khe->hqk', mixed_grad, value_split)
        value_sum = value_sum + pair_product('hqk,qhe->khe', weights, mixed_grad)
        first_grad = prob_maps[:, 0] * (weight_grad - lax.optimization_barrier(jnp.sum(weight_grad * prob_maps[:, 0], axis=-1, keepdims=True)))
        second_grad = -lambda_col * prob_maps[:, 1] * (weight_grad - lax.optimization_barrier(jnp.sum(weight_grad * prob_maps[:, 1], axis=-1, keepdims=True)))
        score_grad = (jnp.stack([first_grad, second_grad], axis=1) * inv_root).astype(jnp.bfloat16)
        query_grad = pair_product('hmqk,khmd->qhmd', score_grad, key_split)
        key_sum = key_sum + pair_product('hmqk,qhmd->khmd', score_grad, query_part)
        return ((key_sum, value_sum), query_grad)
    zero_init = (jnp.zeros((seq_length, head_count, 2, qk_width), jnp.float32), jnp.zeros((seq_length, head_count, value_width), jnp.float32))
    block_starts = jnp.arange(block_count, dtype=jnp.int32) * block_rows
    (key_sum, value_sum), query_blocks = lax.scan(block_step, zero_init, (query_split, grad_split, block_starts))
    query_turned = query_blocks.reshape(seq_length, head_count * 2 * qk_width)
    key_turned = key_sum.reshape(seq_length, head_count * 2 * qk_width)
    query_back = rotate(query_turned, cosine, sine_table, qk_width, -1.0).astype(jnp.bfloat16)
    key_back = rotate(key_turned, cosine, sine_table, qk_width, -1.0).astype(jnp.bfloat16)
    values_back = value_sum.reshape(seq_length, head_count * value_width).astype(jnp.bfloat16)
    return (query_back, key_back, values_back)

def reference(tokens, query_weight, key_weight, values, lambdas, out_grad):
    cosine, sine_table = rotation_tables(jnp.arange(SEQLEN, dtype=jnp.int32), DQK)
    query_float = query_weight.astype(jnp.float32)
    key_float = key_weight.astype(jnp.float32)

    def one_sequence(inputs):
        token_seq, value_seq, grad_seq = inputs
        token_float = token_seq.astype(jnp.float32)
        query_rot = rotate(jnp.dot(token_float, query_float), cosine, sine_table, DQK, 1.0).astype(jnp.bfloat16)
        key_rot = rotate(jnp.dot(token_float, key_float), cosine, sine_table, DQK, 1.0).astype(jnp.bfloat16)
        query_back, key_back, values_back = head_backward(query_rot, key_rot, value_seq, grad_seq, lambdas, cosine, sine_table)
        query_back_f = query_back.astype(jnp.float32)
        key_back_f = key_back.astype(jnp.float32)
        input_grad = (jnp.dot(query_back_f, query_float.T) + jnp.dot(key_back_f, key_float.T)).astype(jnp.bfloat16)
        query_part = jnp.dot(token_float.T, query_back_f)
        key_part = jnp.dot(token_float.T, key_back_f)
        return (input_grad, values_back, query_part, key_part)
    tokens_grad, values_grad, query_parts, key_parts = lax.map(one_sequence, (tokens, values, out_grad))
    factor = 1.0 / math.sqrt(BATCH * SEQLEN)
    return (tokens_grad, values_grad, lax.optimization_barrier(jnp.sum(query_parts, axis=0)) * factor, lax.optimization_barrier(jnp.sum(key_parts, axis=0)) * factor)
```

```python
import functools
import math

import jax
import jax.numpy as jnp
from jax import lax
from jax.experimental import pallas as pl
from jax.experimental.pallas import tpu as pltpu
from jax.sharding import PartitionSpec as P

DQK = 32
NORM_EPS = 0.1
THETA = 10000.0
F32 = jnp.float32
BF16 = jnp.bfloat16


def dot(a, b, ca=1, cb=0):
    return lax.dot_general(a, b, (((ca,), (cb,)), ((), ())), preferred_element_type=F32)


def rotation_tables(seq_length):
    half = DQK // 2
    freqs = jnp.exp(-math.log(THETA) * jnp.arange(half, dtype=F32) / half)
    angles = freqs[:, None] * jnp.arange(seq_length, dtype=jnp.int32).astype(F32)[None, :]
    return jnp.cos(angles), jnp.sin(angles)


def rotate_rows(x, cos, sin):
    half = DQK // 2
    parts = []
    for g in range(x.shape[0] // DQK):
        a = x[g * DQK : g * DQK + half]
        b = x[g * DQK + half : (g + 1) * DQK]
        parts += [a * cos - b * sin, b * cos + a * sin]
    return jnp.concatenate(parts, axis=0)


def attention_kernel(heads, lam_ref, cos_ref, sin_ref, qk_ref, v_ref, og_ref, back_ref, dv_ref,
                     vt_s, ogt_s, dvt_s, dk_s):
    seq = cos_ref.shape[1]
    qc = qk_ref.shape[0] // 2
    hw = qc // heads
    ve = v_ref.shape[1] // heads
    inv_root = 1.0 / math.sqrt(DQK)
    vt_s[...] = v_ref[...].T
    ogt_s[...] = og_ref[...].T
    step = 256

    def one_head(h, _):
        lam = lam_ref[h]
        cos, sin = cos_ref[...], sin_ref[...]
        qrow = pl.multiple_of(h * hw, hw)
        vrow = pl.multiple_of(h * ve, ve)
        qt = rotate_rows(qk_ref[pl.ds(qrow, hw), :], cos, sin).astype(BF16)
        kt = rotate_rows(qk_ref[pl.ds(qc + qrow, hw), :], cos, sin).astype(BF16)
        k = kt.T
        vt = vt_s[pl.ds(vrow, ve), :]
        v = vt.T
        zero_half = jnp.zeros((DQK, step), BF16)
        dk_s[...] = jnp.zeros_like(dk_s)
        dvt_s[pl.ds(vrow, ve), :] = jnp.zeros((ve, seq), F32)
        for t0 in range(0, seq, step):
            end = min(t0 + step, seq)
            tb = end - t0
            zh = zero_half[:, :tb]
            q_b = qt[:, t0:end]
            mask = lax.broadcasted_iota(jnp.int32, (tb, tb), 0) <= lax.broadcasted_iota(
                jnp.int32, (tb, tb), 1
            )
            probs = []
            for m in range(2):
                half_q = q_b[m * DQK : (m + 1) * DQK]
                rhs = jnp.concatenate([half_q, zh] if m == 0 else [zh, half_q], axis=0)
                s = dot(k[:end], rhs) * inv_root
                diag = jnp.where(mask, s[t0:], -jnp.inf)
                s = jnp.concatenate([s[:t0], diag], axis=0) if t0 else diag
                e = jnp.exp(s - jnp.max(s, axis=0, keepdims=True))
                probs.append(e * (1.0 / jnp.sum(e, axis=0, keepdims=True)))
            p1, p2 = probs
            mix = (p1 - lam * p2).astype(BF16)
            ho = dot(vt[:, :end], mix)
            inv = lax.rsqrt(jnp.mean(ho * ho, axis=0, keepdims=True) + NORM_EPS)
            og = ogt_s[pl.ds(vrow, ve), t0:end].astype(F32)
            ob = (inv * og - inv * inv * inv * ho * jnp.mean(og * ho, axis=0, keepdims=True)).astype(BF16)
            mg = dot(v[:end], ob) * inv_root
            g1 = (p1 * (mg - jnp.sum(mg * p1, axis=0, keepdims=True))).astype(BF16)
            g2 = ((-lam * p2) * (mg - jnp.sum(mg * p2, axis=0, keepdims=True))).astype(BF16)
            dvt_s[pl.ds(vrow, ve), :end] += dot(ob, mix, 1, 1)
            dq = jnp.concatenate([dot(kt[:DQK, :end], g1), dot(kt[DQK:, :end], g2)], axis=0)
            back_ref[pl.ds(qrow, hw), t0:end] = rotate_rows(dq, cos[:, t0:end], -sin[:, t0:end]).astype(BF16)
            dk_s[:DQK, :end] += dot(q_b[:DQK], g1, 1, 1)
            dk_s[DQK:, :end] += dot(q_b[DQK:], g2, 1, 1)
        back_ref[pl.ds(qc + qrow, hw), :] = rotate_rows(dk_s[...], cos, -sin).astype(BF16)
        return 0

    lax.fori_loop(0, heads, one_head, 0)
    dv_ref[...] = dvt_s[...].T.astype(BF16)


def attention(qkt, v_all, og_all, lam, cos, sin):
    heads = lam.shape[0]
    seq = v_all.shape[0]
    vc = v_all.shape[1]
    vm = pl.BlockSpec(memory_space=pltpu.VMEM)
    return pl.pallas_call(
        functools.partial(attention_kernel, heads),
        out_shape=(
            jax.ShapeDtypeStruct(qkt.shape, BF16),
            jax.ShapeDtypeStruct(v_all.shape, BF16),
        ),
        in_specs=[pl.BlockSpec(memory_space=pltpu.SMEM)] + [vm] * 5,
        out_specs=(vm, vm),
        scratch_shapes=[
            pltpu.VMEM((vc, seq), BF16),
            pltpu.VMEM((vc, seq), BF16),
            pltpu.VMEM((vc, seq), F32),
            pltpu.VMEM((qkt.shape[0] // heads // 2, seq), F32),
        ],
        compiler_params=pltpu.CompilerParams(vmem_limit_bytes=60 * 1024 * 1024),
        name="attn",
    )(lam, cos, sin, qkt, v_all, og_all)


def body(tokens, query_weight, key_weight, values, lambdas, out_grad):
    sp = lax.axis_size("sp")
    dp = lax.axis_size("dp")
    rows = tokens.shape[1]
    seq = rows * sp
    heads = lambdas.shape[0] // sp
    qc = query_weight.shape[1] // sp
    me = lax.axis_index("sp")
    lam = lax.dynamic_slice_in_dim(lambdas, me * heads, heads)
    cos, sin = rotation_tables(seq)
    w_loc = jnp.concatenate(
        [lax.dynamic_slice_in_dim(w, me * qc, qc, axis=1) for w in (query_weight, key_weight)], axis=1
    )
    w_all = lax.all_gather(w_loc, "dp", axis=0, tiled=True)
    tok_all = lax.all_gather(tokens[0], "sp", axis=0, tiled=True)
    v_all = lax.all_to_all(values[0], "sp", split_axis=1, concat_axis=0, tiled=True)
    og_all = lax.all_to_all(out_grad[0], "sp", split_axis=1, concat_axis=0, tiled=True)
    qkt = dot(w_all, tok_all, 0, 1)
    back, dv = attention(qkt, v_all, og_all, lam, cos, sin)
    wgrad = dot(tok_all, back, 0, 1).astype(BF16)
    tgrad = dot(back, w_all, 0, 1).astype(BF16)
    wshard = lax.psum_scatter(wgrad, "dp", scatter_dimension=0, tiled=True)
    tokens_grad = lax.psum_scatter(tgrad, "sp", scatter_dimension=0, tiled=True)
    values_grad = lax.all_to_all(dv, "sp", split_axis=0, concat_axis=1, tiled=True)
    wfull = lax.all_gather(wshard, "sp", axis=0)
    wfull = jnp.transpose(wfull, (1, 0, 2)).astype(F32) * (1.0 / math.sqrt(dp * seq))
    n = wfull.shape[0]
    qg = wfull[:, :, :qc].reshape(n, sp * qc)
    kg = wfull[:, :, qc:].reshape(n, sp * qc)
    return tokens_grad[None], values_grad[None], qg, kg


def solution(mesh):
    x = P("dp", "sp", None)
    w = P("dp", None)
    return jax.shard_map(
        body, mesh=mesh, in_specs=(x, w, w, x, P(), x), out_specs=(x, x, w, w), check_vma=False
    )
```

```python
import functools
import math

import jax
import jax.numpy as jnp
from jax import lax
from jax.experimental import pallas as pl
from jax.experimental.pallas import tpu as pltpu
from jax.sharding import PartitionSpec as P

DQK = 32
NORM_EPS = 0.1
THETA = 10000.0
F32 = jnp.float32
BF16 = jnp.bfloat16


def dot(a, b, ca=1, cb=0):
    return lax.dot_general(a, b, (((ca,), (cb,)), ((), ())), preferred_element_type=F32)


def rotation_tables(seq_length):
    half = DQK // 2
    freqs = jnp.exp(-math.log(THETA) * jnp.arange(half, dtype=F32) / half)
    angles = freqs[:, None] * jnp.arange(seq_length, dtype=jnp.int32).astype(F32)[None, :]
    return jnp.cos(angles), jnp.sin(angles)


def rotate_rows(x, cos, sin):
    half = DQK // 2
    parts = []
    for g in range(x.shape[0] // DQK):
        a = x[g * DQK : g * DQK + half]
        b = x[g * DQK + half : (g + 1) * DQK]
        parts += [a * cos - b * sin, b * cos + a * sin]
    return jnp.concatenate(parts, axis=0)


def attention_kernel(heads, lam_ref, cos_ref, sin_ref, qk_in, vog_ref, back_ref, rows_ref, dv_ref,
                     qk_ref, vt_s, ogt_s, dvt_s, dk_s):
    seq = cos_ref.shape[1]
    qc = qk_ref.shape[0] // 2
    hw = qc // heads
    ve = vog_ref.shape[2] // heads
    qk_ref[...] = qk_in[...].T
    inv_root = 1.0 / math.sqrt(DQK)
    vt_s[...] = vog_ref[0].T
    ogt_s[...] = vog_ref[1].T
    step = 256

    def one_head(h, _):
        lam = lam_ref[h]
        cos, sin = cos_ref[...], sin_ref[...]
        qrow = pl.multiple_of(h * hw, hw)
        vrow = pl.multiple_of(h * ve, ve)
        qt = rotate_rows(qk_ref[pl.ds(qrow, hw), :], cos, sin).astype(BF16)
        kt = rotate_rows(qk_ref[pl.ds(qc + qrow, hw), :], cos, sin).astype(BF16)
        k = kt.T
        vt = vt_s[pl.ds(vrow, ve), :]
        v = vt.T
        zero_half = jnp.zeros((DQK, step), BF16)
        dk_s[...] = jnp.zeros_like(dk_s)
        dvt_s[pl.ds(vrow, ve), :] = jnp.zeros((ve, seq), F32)
        for t0 in range(0, seq, step):
            end = min(t0 + step, seq)
            tb = end - t0
            zh = zero_half[:, :tb]
            q_b = qt[:, t0:end]
            mask = lax.broadcasted_iota(jnp.int32, (tb, tb), 0) <= lax.broadcasted_iota(
                jnp.int32, (tb, tb), 1
            )
            probs = []
            for m in range(2):
                half_q = q_b[m * DQK : (m + 1) * DQK]
                rhs = jnp.concatenate([half_q, zh] if m == 0 else [zh, half_q], axis=0)
                s = dot(k[:end], rhs) * inv_root
                diag = jnp.where(mask, s[t0:], -jnp.inf)
                s = jnp.concatenate([s[:t0], diag], axis=0) if t0 else diag
                e = jnp.exp(s - jnp.max(s, axis=0, keepdims=True))
                probs.append(e * (1.0 / jnp.sum(e, axis=0, keepdims=True)))
            p1, p2 = probs
            mix = (p1 - lam * p2).astype(BF16)
            ho = dot(vt[:, :end], mix)
            inv = lax.rsqrt(jnp.mean(ho * ho, axis=0, keepdims=True) + NORM_EPS)
            og = ogt_s[pl.ds(vrow, ve), t0:end].astype(F32)
            ob = (inv * og - inv * inv * inv * ho * jnp.mean(og * ho, axis=0, keepdims=True)).astype(BF16)
            mg = dot(v[:end], ob) * inv_root
            g1 = (p1 * (mg - jnp.sum(mg * p1, axis=0, keepdims=True))).astype(BF16)
            g2 = ((-lam * p2) * (mg - jnp.sum(mg * p2, axis=0, keepdims=True))).astype(BF16)
            dvt_s[pl.ds(vrow, ve), :end] += dot(ob, mix, 1, 1)
            dq = jnp.concatenate([dot(kt[:DQK, :end], g1), dot(kt[DQK:, :end], g2)], axis=0)
            back_ref[pl.ds(qrow, hw), t0:end] = rotate_rows(dq, cos[:, t0:end], -sin[:, t0:end]).astype(BF16)
            dk_s[:DQK, :end] += dot(q_b[:DQK], g1, 1, 1)
            dk_s[DQK:, :end] += dot(q_b[DQK:], g2, 1, 1)
        back_ref[pl.ds(qc + qrow, hw), :] = rotate_rows(dk_s[...], cos, -sin).astype(BF16)
        return 0

    lax.fori_loop(0, heads, one_head, 0)
    dv_ref[...] = dvt_s[...].T.astype(BF16)
    rows_ref[...] = back_ref[...].T


def attention(qk, vog, lam, cos, sin):
    heads = lam.shape[0]
    seq, qk_cols = qk.shape
    vc = vog.shape[2]
    vm = pl.BlockSpec(memory_space=pltpu.VMEM)
    return pl.pallas_call(
        functools.partial(attention_kernel, heads),
        out_shape=(
            jax.ShapeDtypeStruct((qk_cols, seq), BF16),
            jax.ShapeDtypeStruct((seq, qk_cols), BF16),
            jax.ShapeDtypeStruct((seq, vc), BF16),
        ),
        in_specs=[pl.BlockSpec(memory_space=pltpu.SMEM)] + [vm] * 4,
        out_specs=(vm, vm, vm),
        scratch_shapes=[
            pltpu.VMEM((qk_cols, seq), F32),
            pltpu.VMEM((vc, seq), BF16),
            pltpu.VMEM((vc, seq), BF16),
            pltpu.VMEM((vc, seq), F32),
            pltpu.VMEM((qk_cols // heads // 2, seq), F32),
        ],
        compiler_params=pltpu.CompilerParams(vmem_limit_bytes=60 * 1024 * 1024),
        name="attn",
    )(lam, cos, sin, qk, vog)


def sender(src, dst, ssem, rsem, device):
    return pltpu.make_async_remote_copy(
        src_ref=src, dst_ref=dst, send_sem=ssem, recv_sem=rsem,
        device_id=device, device_id_type=pl.DeviceIdType.MESH,
    )


def places(sp, dp):
    me, mine = lax.axis_index("sp"), lax.axis_index("dp")
    z, core = mine // 2, lax.rem(mine, 2)
    nz = dp // 2
    if sp == 4:
        peers = [me + 1 - 2 * lax.rem(me, 2), lax.rem(me + 2, 4), 3 - me]
        froms = peers
    else:
        peers = [lax.rem(me + d, sp) for d in range(1, sp)]
        froms = [lax.rem(me + sp - d, sp) for d in range(1, sp)]
    z_to = [lax.rem(z + i, nz) * 2 for i in range(1, nz)]
    z_from = [lax.rem(z + nz - i, nz) * 2 for i in range(1, nz)]
    return me, mine, z, core, peers, froms, z_to, z_from


def greet(me, mine, core, peers, z_to):
    barrier = pltpu.get_barrier_semaphore()
    where = [(p, mine) for p in peers] + [(me, zt + core) for zt in z_to] + [(me, mine + 1 - 2 * core)]
    for device in where:
        pl.semaphore_signal(barrier, inc=1, device_id=device, device_id_type=pl.DeviceIdType.MESH)
    pl.semaphore_wait(barrier, len(where))


def gather_kernel(sp, dp, tok_ref, vog_ref, w_ref, tok_all, vog_all, w_all, qk_ref,
                  tok_ss, tok_rs, vog_ss, vog_rs, w_ss, w_rs, sib_ss, sib_rs):
    me, mine, z, core, peers, froms, z_to, z_from = places(sp, dp)
    rows, wr = tok_ref.shape[0], w_ref.shape[0]
    sib = (me, mine + 1 - 2 * core)
    greet(me, mine, core, peers, z_to)

    def trow(i, start=0, size=rows):
        return pl.ds(pl.multiple_of(i * rows + start, 16), size)

    def wrow(i):
        return pl.ds(pl.multiple_of(i * wr, wr), wr)

    sends = []

    def go(copy):
        copy.start()
        sends.append(copy)
        return copy

    wz = [go(sender(w_ref, w_all.at[wrow(mine)], w_ss.at[i], w_rs.at[i], (me, zt + core)))
          for i, zt in enumerate(z_to)]
    ws = [go(sender(w_ref, w_all.at[wrow(mine)], sib_ss.at[0], sib_rs.at[0], sib))]
    half = rows // 2
    if sp == 4:
        def piece(p, h, k):
            r = trow(me, h * half, half)
            return go(sender(tok_ref.at[pl.ds(h * half, half)], tok_all.at[r], tok_ss.at[k], tok_rs.at[k], (p, mine)))

        x0, y1 = piece(peers[0], 0, 0), piece(peers[1], 1, 1)
        x1, y0 = piece(peers[0], 1, 2), piece(peers[1], 0, 3)
    else:
        tk = [go(sender(tok_ref, tok_all.at[trow(me)], tok_ss.at[i], tok_rs.at[i], (p, mine)))
              for i, p in enumerate(peers)]
    vg = [go(sender(vog_ref.at[p], vog_all.at[:, trow(me)], vog_ss.at[i], vog_rs.at[i], (p, mine)))
          for i, p in enumerate(peers)]
    tok_all[trow(me), :] = tok_ref[...]
    vog_all[:, trow(me), :] = vog_ref[me]
    w_all[wrow(mine), :] = w_ref[...]
    if sp == 4:
        x0.wait_recv()
        f0 = trow(peers[0], 0, half)
        d0 = go(sender(tok_all.at[f0], tok_all.at[f0], tok_ss.at[4], tok_rs.at[4], (peers[1], mine)))
        y1.wait_recv()
        f1 = trow(peers[1], half, half)
        d1 = go(sender(tok_all.at[f1], tok_all.at[f1], tok_ss.at[5], tok_rs.at[5], (peers[0], mine)))
        arrivals = [[x1], [y0], [d0, d1]]
    else:
        arrivals = [[c] for c in tk]
    for i, zf in enumerate(z_from):
        wz[i].wait_recv()
        r = wrow(zf + core)
        ws.append(go(sender(w_all.at[r], w_all.at[r], sib_ss.at[i + 1], sib_rs.at[i + 1], sib)))
    for c in ws:
        c.wait_recv()
    qk_ref[trow(me), :] = dot(tok_ref[...], w_all[...])
    for f, copies in zip(froms, arrivals):
        for c in copies:
            c.wait_recv()
        qk_ref[trow(f), :] = dot(tok_all[trow(f), :], w_all[...])
    for c in vg:
        c.wait_recv()
    for c in sends:
        c.wait_send()


def gather(tok, vog, w, sp, dp):
    rows, width = tok.shape
    vm = pl.BlockSpec(memory_space=pltpu.VMEM)
    dma = pltpu.SemaphoreType.DMA
    nt = 6 if sp == 4 else sp - 1
    nz = dp // 2
    return pl.pallas_call(
        functools.partial(gather_kernel, sp, dp),
        out_shape=(
            jax.ShapeDtypeStruct((rows * sp, width), BF16),
            jax.ShapeDtypeStruct((2, rows * sp, vog.shape[3]), BF16),
            jax.ShapeDtypeStruct((w.shape[0] * dp, w.shape[1]), BF16),
            jax.ShapeDtypeStruct((rows * sp, w.shape[1]), F32),
        ),
        in_specs=[vm] * 3,
        out_specs=(vm,) * 4,
        scratch_shapes=[dma((nt,)), dma((nt,)), dma((sp - 1,)), dma((sp - 1,)),
                        dma((nz - 1,)), dma((nz - 1,)), dma((nz,)), dma((nz,))],
        compiler_params=pltpu.CompilerParams(
            vmem_limit_bytes=60 * 1024 * 1024, collective_id=0, has_side_effects=True
        ),
        name="gather",
    )(tok, vog, w)


def scatter_kernel(sp, dp, factor, back_t, back_m, tok_all, w_all, dv, tg_out, dv_out, qg, kg,
                   tbuf, trecv, tacc, dvr, sib_s, sib_r, wz_s, wz_r, wacc, wg_s, wg_r,
                   t_ss, t_rs, d_ss, d_rs, s_ss, s_rs, z_ss, z_rs, g_ss, g_rs):
    me, mine, z, core, peers, froms, z_to, z_from = places(sp, dp)
    nz = dp // 2
    rows, wr = tg_out.shape[0], qg.shape[0]
    vc = dv.shape[1]
    qc = w_all.shape[1] // 2
    sib = (me, mine + 1 - 2 * core)
    greet(me, mine, core, peers, z_to)
    sends = []

    def go(copy):
        copy.start()
        sends.append(copy)
        return copy

    def trow(i):
        return pl.ds(pl.multiple_of(i * rows, 16), rows)

    def weight_part(owner):
        return dot(back_t[...], tok_all[:, pl.ds(pl.multiple_of(owner * wr, wr), wr)])

    def token_part(p):
        return dot(back_m[trow(p), :], w_all[...], 1, 1)

    def send_tokens(i):
        tbuf[i] = token_part(peers[i]).astype(BF16)
        return go(sender(tbuf.at[i], trecv.at[i], t_ss.at[i], t_rs.at[i], (peers[i], mine)))

    targets = z_to + [z * 2]
    tg = [send_tokens(0)]
    sb = []
    for i, zt in enumerate(targets):
        sib_s[i] = weight_part(zt + 1 - core).astype(BF16)
        sb.append(go(sender(sib_s.at[i], sib_r.at[i], s_ss.at[i], s_rs.at[i], sib)))
    zs = []
    for i, zt in enumerate(targets):
        part = weight_part(zt + core)
        sb[i].wait_recv()
        part = part + sib_r[i].astype(F32)
        if i < nz - 1:
            wz_s[i] = part.astype(BF16)
            zs.append(go(sender(wz_s.at[i], wz_r.at[i], z_ss.at[i], z_rs.at[i], (me, zt + core))))
        else:
            wacc[...] = part
    for i in range(1, sp - 1):
        tg.append(send_tokens(i))
    dvc = [go(sender(dv.at[trow(p)], dvr.at[me], d_ss.at[i], d_rs.at[i], (p, mine)))
           for i, p in enumerate(peers)]
    dvr[me] = dv[trow(me), :]
    tacc[...] = token_part(me)
    for i in range(nz - 1):
        zs[i].wait_recv()
        wacc[...] += wz_r[i].astype(F32)
    total = wacc[...].T.astype(BF16)
    wg_s[...] = total
    gs = [go(sender(wg_s, wg_r.at[me], g_ss.at[i], g_rs.at[i], (p, mine))) for i, p in enumerate(peers)]
    wg_r[me] = total
    for i in range(sp - 1):
        tg[i].wait_recv()
        tacc[...] += trecv[i].astype(F32)
    tg_out[...] = tacc[...].astype(BF16)
    for c in dvc:
        c.wait_recv()
    for s in range(sp):
        dv_out[:, s * vc : (s + 1) * vc] = dvr[s]
    for c in gs:
        c.wait_recv()
    for s in range(sp):
        qg[:, s * qc : (s + 1) * qc] = wg_r[s, :, :qc].astype(F32) * factor
        kg[:, s * qc : (s + 1) * qc] = wg_r[s, :, qc:].astype(F32) * factor
    for c in sends:
        c.wait_send()


def scatter(back_t, back_m, tok_all, w_all, dv, sp, dp):
    seq, width = tok_all.shape
    rows, wr = seq // sp, width // dp
    cols = w_all.shape[1]
    vc = dv.shape[1]
    nz = dp // 2
    vm = pl.BlockSpec(memory_space=pltpu.VMEM)
    dma = pltpu.SemaphoreType.DMA
    factor = 1.0 / math.sqrt(dp * seq)
    return pl.pallas_call(
        functools.partial(scatter_kernel, sp, dp, factor),
        out_shape=(
            jax.ShapeDtypeStruct((rows, width), BF16),
            jax.ShapeDtypeStruct((rows, vc * sp), BF16),
            jax.ShapeDtypeStruct((wr, cols // 2 * sp), F32),
            jax.ShapeDtypeStruct((wr, cols // 2 * sp), F32),
        ),
        in_specs=[vm] * 5,
        out_specs=(vm,) * 4,
        scratch_shapes=[
            pltpu.VMEM((sp - 1, rows, width), BF16),
            pltpu.VMEM((sp - 1, rows, width), BF16),
            pltpu.VMEM((rows, width), F32),
            pltpu.VMEM((sp, rows, vc), BF16),
            pltpu.VMEM((nz, cols, wr), BF16),
            pltpu.VMEM((nz, cols, wr), BF16),
            pltpu.VMEM((nz - 1, cols, wr), BF16),
            pltpu.VMEM((nz - 1, cols, wr), BF16),
            pltpu.VMEM((cols, wr), F32),
            pltpu.VMEM((wr, cols), BF16),
            pltpu.VMEM((sp, wr, cols), BF16),
            dma((sp - 1,)), dma((sp - 1,)), dma((sp - 1,)), dma((sp - 1,)), dma((nz,)), dma((nz,)),
            dma((nz - 1,)), dma((nz - 1,)), dma((sp - 1,)), dma((sp - 1,)),
        ],
        compiler_params=pltpu.CompilerParams(
            vmem_limit_bytes=62 * 1024 * 1024, collective_id=1, has_side_effects=True
        ),
        name="scatter",
    )(back_t, back_m, tok_all, w_all, dv)


def body(tokens, query_weight, key_weight, values, lambdas, out_grad):
    sp = lax.axis_size("sp")
    dp = lax.axis_size("dp")
    rows = tokens.shape[1]
    heads = lambdas.shape[0] // sp
    qc = query_weight.shape[1] // sp
    me = lax.axis_index("sp")
    lam = lax.dynamic_slice_in_dim(lambdas, me * heads, heads)
    cos, sin = rotation_tables(rows * sp)
    w_loc = jnp.concatenate(
        [lax.dynamic_slice_in_dim(w, me * qc, qc, axis=1) for w in (query_weight, key_weight)], axis=1
    )
    vog = jnp.stack([values[0], out_grad[0]]).reshape(2, rows, sp, -1).transpose(2, 0, 1, 3)
    tok_all, vog_all, w_all, qk = gather(tokens[0], vog, w_loc, sp, dp)
    back_t, back_m, dv = attention(qk, vog_all, lam, cos, sin)
    tokens_grad, values_grad, qg, kg = scatter(back_t, back_m, tok_all, w_all, dv, sp, dp)
    return tokens_grad[None], values_grad[None], qg, kg


def solution(mesh):
    x = P("dp", "sp", None)
    w = P("dp", None)
    return jax.shard_map(
        body, mesh=mesh, in_specs=(x, w, w, x, P(), x), out_specs=(x, x, w, w), check_vma=False
    )
```

```python
import functools
import math

import jax
import jax.numpy as jnp
from jax import lax
from jax.experimental import pallas as pl
from jax.experimental.pallas import tpu as pltpu
from jax.sharding import PartitionSpec as P

DQK = 32
NORM_EPS = 0.1
THETA = 10000.0
F32 = jnp.float32
BF16 = jnp.bfloat16


def dot(a, b, ca=1, cb=0):
    return lax.dot_general(a, b, (((ca,), (cb,)), ((), ())), preferred_element_type=F32)


def rotation_tables(seq_length):
    half = DQK // 2
    freqs = jnp.exp(-math.log(THETA) * jnp.arange(half, dtype=F32) / half)
    angles = freqs[:, None] * jnp.arange(seq_length, dtype=jnp.int32).astype(F32)[None, :]
    return jnp.cos(angles), jnp.sin(angles)


def rotate_rows(x, cos, sin):
    half = DQK // 2
    parts = []
    for g in range(x.shape[0] // DQK):
        a = x[g * DQK : g * DQK + half]
        b = x[g * DQK + half : (g + 1) * DQK]
        parts += [a * cos - b * sin, b * cos + a * sin]
    return jnp.concatenate(parts, axis=0)


def attention_kernel(heads, lam_ref, cos_ref, sin_ref, qk_in, vog_ref, back_ref, rows_ref, dv_ref,
                     qk_ref, vt_s, ogt_s, dvt_s, dk_s):
    seq = cos_ref.shape[1]
    qc = qk_ref.shape[0] // 2
    hw = qc // heads
    ve = vog_ref.shape[2] // heads
    qk_ref[...] = qk_in[...].T
    inv_root = 1.0 / math.sqrt(DQK)
    vt_s[...] = vog_ref[0].T
    ogt_s[...] = vog_ref[1].T
    step = 256

    def one_head(h, _):
        lam = lam_ref[lax.axis_index("sp") * heads + h]
        cos, sin = cos_ref[...], sin_ref[...]
        qrow = pl.multiple_of(h * hw, hw)
        vrow = pl.multiple_of(h * ve, ve)
        qt = rotate_rows(qk_ref[pl.ds(qrow, hw), :], cos, sin).astype(BF16)
        kt = rotate_rows(qk_ref[pl.ds(qc + qrow, hw), :], cos, sin).astype(BF16)
        k = kt.T
        vt = vt_s[pl.ds(vrow, ve), :]
        v = vt.T
        zero_half = jnp.zeros((DQK, step), BF16)
        dk_s[...] = jnp.zeros_like(dk_s)
        dvt_s[pl.ds(vrow, ve), :] = jnp.zeros((ve, seq), F32)
        for t0 in range(0, seq, step):
            end = min(t0 + step, seq)
            tb = end - t0
            zh = zero_half[:, :tb]
            q_b = qt[:, t0:end]
            mask = lax.broadcasted_iota(jnp.int32, (tb, tb), 0) <= lax.broadcasted_iota(
                jnp.int32, (tb, tb), 1
            )
            probs = []
            for m in range(2):
                half_q = q_b[m * DQK : (m + 1) * DQK]
                rhs = jnp.concatenate([half_q, zh] if m == 0 else [zh, half_q], axis=0)
                s = dot(k[:end], rhs) * inv_root
                diag = jnp.where(mask, s[t0:], -jnp.inf)
                s = jnp.concatenate([s[:t0], diag], axis=0) if t0 else diag
                e = jnp.exp(s - jnp.max(s, axis=0, keepdims=True))
                probs.append(e * (1.0 / jnp.sum(e, axis=0, keepdims=True)))
            p1, p2 = probs
            mix = (p1 - lam * p2).astype(BF16)
            ho = dot(vt[:, :end], mix)
            inv = lax.rsqrt(jnp.mean(ho * ho, axis=0, keepdims=True) + NORM_EPS)
            og = ogt_s[pl.ds(vrow, ve), t0:end].astype(F32)
            ob = (inv * og - inv * inv * inv * ho * jnp.mean(og * ho, axis=0, keepdims=True)).astype(BF16)
            mg = dot(v[:end], ob) * inv_root
            g1 = (p1 * (mg - jnp.sum(mg * p1, axis=0, keepdims=True))).astype(BF16)
            g2 = ((-lam * p2) * (mg - jnp.sum(mg * p2, axis=0, keepdims=True))).astype(BF16)
            dvt_s[pl.ds(vrow, ve), :end] += dot(ob, mix, 1, 1)
            dq = jnp.concatenate([dot(kt[:DQK, :end], g1), dot(kt[DQK:, :end], g2)], axis=0)
            back_ref[pl.ds(qrow, hw), t0:end] = rotate_rows(dq, cos[:, t0:end], -sin[:, t0:end]).astype(BF16)
            dk_s[:DQK, :end] += dot(q_b[:DQK], g1, 1, 1)
            dk_s[DQK:, :end] += dot(q_b[DQK:], g2, 1, 1)
        back_ref[pl.ds(qc + qrow, hw), :] = rotate_rows(dk_s[...], cos, -sin).astype(BF16)
        return 0

    lax.fori_loop(0, heads, one_head, 0)
    dv_ref[...] = dvt_s[...].T.astype(BF16)
    rows_ref[...] = back_ref[...].T


def attention(qk, vog, lam, cos, sin, heads):
    seq, qk_cols = qk.shape
    vc = vog.shape[2]
    vm = pl.BlockSpec(memory_space=pltpu.VMEM)
    return pl.pallas_call(
        functools.partial(attention_kernel, heads),
        out_shape=(
            jax.ShapeDtypeStruct((qk_cols, seq), BF16),
            jax.ShapeDtypeStruct((seq, qk_cols), BF16),
            jax.ShapeDtypeStruct((seq, vc), BF16),
        ),
        in_specs=[pl.BlockSpec(memory_space=pltpu.SMEM)] + [vm] * 4,
        out_specs=(vm, vm, vm),
        scratch_shapes=[
            pltpu.VMEM((qk_cols, seq), F32),
            pltpu.VMEM((vc, seq), BF16),
            pltpu.VMEM((vc, seq), BF16),
            pltpu.VMEM((vc, seq), F32),
            pltpu.VMEM((qk_cols // heads // 2, seq), F32),
        ],
        compiler_params=pltpu.CompilerParams(vmem_limit_bytes=60 * 1024 * 1024),
        name="attn",
    )(lam, cos, sin, qk, vog)


def sender(src, dst, ssem, rsem, device):
    return pltpu.make_async_remote_copy(
        src_ref=src, dst_ref=dst, send_sem=ssem, recv_sem=rsem,
        device_id=device, device_id_type=pl.DeviceIdType.MESH,
    )


def places(sp, dp):
    me, mine = lax.axis_index("sp"), lax.axis_index("dp")
    z, core = mine // 2, lax.rem(mine, 2)
    nz = dp // 2
    if sp == 4:
        peers = [me + 1 - 2 * lax.rem(me, 2), lax.rem(me + 2, 4), 3 - me]
        froms = peers
    else:
        peers = [lax.rem(me + d, sp) for d in range(1, sp)]
        froms = [lax.rem(me + sp - d, sp) for d in range(1, sp)]
    z_to = [lax.rem(z + i, nz) * 2 for i in range(1, nz)]
    z_from = [lax.rem(z + nz - i, nz) * 2 for i in range(1, nz)]
    return me, mine, z, core, peers, froms, z_to, z_from


def greet(me, mine, core, peers, z_to):
    barrier = pltpu.get_barrier_semaphore()
    where = [(p, mine) for p in peers] + [(me, zt + core) for zt in z_to] + [(me, mine + 1 - 2 * core)]
    for device in where:
        pl.semaphore_signal(barrier, inc=1, device_id=device, device_id_type=pl.DeviceIdType.MESH)
    pl.semaphore_wait(barrier, len(where))


def gather_kernel(sp, dp, tok_ref, v_ref, og_ref, wq_ref, wk_ref, tok_all, vog_all, w_all, qk_ref,
                  vog_ref, tok_ss, tok_rs, vog_ss, vog_rs, w_ss, w_rs, sib_ss, sib_rs):
    me, mine, z, core, peers, froms, z_to, z_from = places(sp, dp)
    rows, wr = tok_ref.shape[0], wq_ref.shape[0]
    sib = (me, mine + 1 - 2 * core)

    def trow(i, start=0, size=rows):
        return pl.ds(pl.multiple_of(i * rows + start, 16), size)

    def wrow(i):
        return pl.ds(pl.multiple_of(i * wr, wr), wr)

    vc, qc = v_ref.shape[1] // sp, wq_ref.shape[1] // sp
    for s in range(sp):
        vog_ref[s, 0] = v_ref[:, s * vc : (s + 1) * vc]
        vog_ref[s, 1] = og_ref[:, s * vc : (s + 1) * vc]

        @pl.when(me == s)
        def _():
            w_all[wrow(mine), :qc] = wq_ref[:, s * qc : (s + 1) * qc]
            w_all[wrow(mine), qc:] = wk_ref[:, s * qc : (s + 1) * qc]

    tok_all[trow(me), :] = tok_ref[...]
    greet(me, mine, core, peers, z_to)
    w_ref = w_all.at[wrow(mine)]
    sends = []

    def go(copy):
        copy.start()
        sends.append(copy)
        return copy

    wz = [go(sender(w_ref, w_all.at[wrow(mine)], w_ss.at[i], w_rs.at[i], (me, zt + core)))
          for i, zt in enumerate(z_to)]
    ws = [go(sender(w_ref, w_all.at[wrow(mine)], sib_ss.at[0], sib_rs.at[0], sib))]
    half = rows // 2
    if sp == 4:
        def piece(p, h, k):
            r = trow(me, h * half, half)
            return go(sender(tok_ref.at[pl.ds(h * half, half)], tok_all.at[r], tok_ss.at[k], tok_rs.at[k], (p, mine)))

        x0, y1 = piece(peers[0], 0, 0), piece(peers[1], 1, 1)
        x1, y0 = piece(peers[0], 1, 2), piece(peers[1], 0, 3)
    else:
        tk = [go(sender(tok_ref, tok_all.at[trow(me)], tok_ss.at[i], tok_rs.at[i], (p, mine)))
              for i, p in enumerate(peers)]
    vg = [go(sender(vog_ref.at[p], vog_all.at[:, trow(me)], vog_ss.at[i], vog_rs.at[i], (p, mine)))
          for i, p in enumerate(peers)]
    vog_all[:, trow(me), :] = vog_ref[me]
    if sp == 4:
        x0.wait_recv()
        f0 = trow(peers[0], 0, half)
        d0 = go(sender(tok_all.at[f0], tok_all.at[f0], tok_ss.at[4], tok_rs.at[4], (peers[1], mine)))
        y1.wait_recv()
        f1 = trow(peers[1], half, half)
        d1 = go(sender(tok_all.at[f1], tok_all.at[f1], tok_ss.at[5], tok_rs.at[5], (peers[0], mine)))
        arrivals = [[x1], [y0], [d0, d1]]
    else:
        arrivals = [[c] for c in tk]
    for i, zf in enumerate(z_from):
        wz[i].wait_recv()
        r = wrow(zf + core)
        ws.append(go(sender(w_all.at[r], w_all.at[r], sib_ss.at[i + 1], sib_rs.at[i + 1], sib)))
    for c in ws:
        c.wait_recv()
    qk_ref[trow(me), :] = dot(tok_ref[...], w_all[...])
    for f, copies in zip(froms, arrivals):
        for c in copies:
            c.wait_recv()
        qk_ref[trow(f), :] = dot(tok_all[trow(f), :], w_all[...])
    for c in vg:
        c.wait_recv()
    for c in sends:
        c.wait_send()


def gather(tok, v, og, wq, wk, sp, dp):
    rows, width = tok.shape
    vc, wr, cols = v.shape[1] // sp, wq.shape[0], 2 * wq.shape[1] // sp
    vm = pl.BlockSpec(memory_space=pltpu.VMEM)
    dma = pltpu.SemaphoreType.DMA
    nt = 6 if sp == 4 else sp - 1
    nz = dp // 2
    return pl.pallas_call(
        functools.partial(gather_kernel, sp, dp),
        out_shape=(
            jax.ShapeDtypeStruct((rows * sp, width), BF16),
            jax.ShapeDtypeStruct((2, rows * sp, vc), BF16),
            jax.ShapeDtypeStruct((wr * dp, cols), BF16),
            jax.ShapeDtypeStruct((rows * sp, cols), F32),
        ),
        in_specs=[vm] * 5,
        out_specs=(vm,) * 4,
        scratch_shapes=[pltpu.VMEM((sp, 2, rows, vc), BF16), dma((nt,)), dma((nt,)), dma((sp - 1,)), dma((sp - 1,)),
                        dma((nz - 1,)), dma((nz - 1,)), dma((nz,)), dma((nz,))],
        compiler_params=pltpu.CompilerParams(
            vmem_limit_bytes=60 * 1024 * 1024, collective_id=0, has_side_effects=True
        ),
        name="gather",
    )(tok, v, og, wq, wk)


def scatter_kernel(sp, dp, back_t, back_m, tok_all, w_all, dv, tg_out, dv_out, qg, kg,
                   tbuf, trecv, tacc, dvr, sib_s, sib_r, wz_s, wz_r, wacc, wg_s, wg_r,
                   t_ss, t_rs, d_ss, d_rs, s_ss, s_rs, z_ss, z_rs, g_ss, g_rs):
    me, mine, z, core, peers, froms, z_to, z_from = places(sp, dp)
    nz = dp // 2
    rows, wr = tg_out.shape[0], qg.shape[0]
    vc = dv.shape[1]
    qc = w_all.shape[1] // 2
    sib = (me, mine + 1 - 2 * core)
    greet(me, mine, core, peers, z_to)
    sends = []

    def go(copy):
        copy.start()
        sends.append(copy)
        return copy

    def trow(i):
        return pl.ds(pl.multiple_of(i * rows, 16), rows)

    def weight_part(owner):
        return dot(back_t[...], tok_all[:, pl.ds(pl.multiple_of(owner * wr, wr), wr)])

    def token_part(p):
        return dot(back_m[trow(p), :], w_all[...], 1, 1)

    def send_tokens(i):
        tbuf[i] = token_part(peers[i]).astype(BF16)
        return go(sender(tbuf.at[i], trecv.at[i], t_ss.at[i], t_rs.at[i], (peers[i], mine)))

    targets = z_to + [z * 2]
    half = rows // 2
    lo, hi = pl.ds(0, half), pl.ds(half, half)
    tg = []

    def hop(i, dst, part, k, to):
        return go(sender(tbuf.at[i, part], trecv.at[dst, part], t_ss.at[k], t_rs.at[k], (peers[to], mine)))

    if sp == 4:
        tbuf[2] = token_part(peers[2]).astype(BF16)
        via_x, via_y = hop(2, 2, lo, 0, 0), hop(2, 2, hi, 1, 1)
    else:
        tg.append(send_tokens(0))
    sb = []
    for i, zt in enumerate(targets):
        sib_s[i] = weight_part(zt + 1 - core).astype(BF16)
        sb.append(go(sender(sib_s.at[i], sib_r.at[i], s_ss.at[i], s_rs.at[i], sib)))
    zs = []
    for i, zt in enumerate(targets):
        part = weight_part(zt + core)
        sb[i].wait_recv()
        part = part + sib_r[i].astype(F32)
        if i < nz - 1:
            wz_s[i] = part.astype(BF16)
            zs.append(go(sender(wz_s.at[i], wz_r.at[i], z_ss.at[i], z_rs.at[i], (me, zt + core))))
        else:
            wacc[...] = part
    if sp == 4:
        part = token_part(peers[0])
        tbuf[0, lo] = part[:half].astype(BF16)
        x_lo = hop(0, 0, lo, 2, 0)
        tacc[hi] = part[half:]
        part = token_part(peers[1])
        tbuf[1, hi] = part[half:].astype(BF16)
        y_hi = hop(1, 1, hi, 3, 1)
        tacc[lo] = part[:half]
        via_x.wait_recv()
        tbuf[1, lo] = (tacc[lo] + trecv[2, lo].astype(F32)).astype(BF16)
        y_lo = hop(1, 1, lo, 4, 1)
        via_y.wait_recv()
        tbuf[0, hi] = (tacc[hi] + trecv[2, hi].astype(F32)).astype(BF16)
        x_hi = hop(0, 0, hi, 5, 0)
        tg = [x_lo, x_hi, y_lo, y_hi]
    else:
        for i in range(1, sp - 1):
            tg.append(send_tokens(i))
    dvc = [go(sender(dv.at[trow(p)], dvr.at[me], d_ss.at[i], d_rs.at[i], (p, mine)))
           for i, p in enumerate(peers)]
    dvr[me] = dv[trow(me), :]
    tacc[...] = token_part(me)
    for i in range(nz - 1):
        zs[i].wait_recv()
        wacc[...] += wz_r[i].astype(F32)
    total = wacc[...].T.astype(BF16)
    wg_s[...] = total
    wg_r[me] = total
    wh = wr // 2
    if sp == 4:
        def piece(p, h, k):
            r = pl.ds(h * wh, wh)
            return go(sender(wg_s.at[r], wg_r.at[me, r], g_ss.at[k], g_rs.at[k], (p, mine)))

        def forward(f, h, k, p):
            r = pl.ds(h * wh, wh)
            return go(sender(wg_r.at[f, r], wg_r.at[f, r], g_ss.at[k], g_rs.at[k], (p, mine)))

        gx0, gy1 = piece(peers[0], 0, 0), piece(peers[1], 1, 1)
        gx1, gy0 = piece(peers[0], 1, 2), piece(peers[1], 0, 3)
        gx0.wait_recv()
        gd0 = forward(peers[0], 0, 4, peers[1])
        gy1.wait_recv()
        gd1 = forward(peers[1], 1, 5, peers[0])
        gs = [gx1, gy0, gd0, gd1]
    else:
        gs = [go(sender(wg_s, wg_r.at[me], g_ss.at[i], g_rs.at[i], (p, mine))) for i, p in enumerate(peers)]
    for c in tg:
        c.wait_recv()
    for i in range(2 if sp == 4 else sp - 1):
        tacc[...] += trecv[i].astype(F32)
    tg_out[...] = tacc[...].astype(BF16)
    for c in dvc:
        c.wait_recv()
    for s in range(sp):
        dv_out[:, s * vc : (s + 1) * vc] = dvr[s]
    for c in gs:
        c.wait_recv()
    for s in range(sp):
        qg[:, s * qc : (s + 1) * qc] = wg_r[s, :, :qc]
        kg[:, s * qc : (s + 1) * qc] = wg_r[s, :, qc:]
    for c in sends:
        c.wait_send()


def scatter(back_t, back_m, tok_all, w_all, dv, sp, dp):
    seq, width = tok_all.shape
    rows, wr = seq // sp, width // dp
    cols = w_all.shape[1]
    vc = dv.shape[1]
    nz = dp // 2
    vm = pl.BlockSpec(memory_space=pltpu.VMEM)
    dma = pltpu.SemaphoreType.DMA
    nt = 6 if sp == 4 else sp - 1
    return pl.pallas_call(
        functools.partial(scatter_kernel, sp, dp),
        out_shape=(
            jax.ShapeDtypeStruct((rows, width), BF16),
            jax.ShapeDtypeStruct((rows, vc * sp), BF16),
            jax.ShapeDtypeStruct((wr, cols // 2 * sp), BF16),
            jax.ShapeDtypeStruct((wr, cols // 2 * sp), BF16),
        ),
        in_specs=[vm] * 5,
        out_specs=(vm,) * 4,
        scratch_shapes=[
            pltpu.VMEM((sp - 1, rows, width), BF16),
            pltpu.VMEM((sp - 1, rows, width), BF16),
            pltpu.VMEM((rows, width), F32),
            pltpu.VMEM((sp, rows, vc), BF16),
            pltpu.VMEM((nz, cols, wr), BF16),
            pltpu.VMEM((nz, cols, wr), BF16),
            pltpu.VMEM((nz - 1, cols, wr), BF16),
            pltpu.VMEM((nz - 1, cols, wr), BF16),
            pltpu.VMEM((cols, wr), F32),
            pltpu.VMEM((wr, cols), BF16),
            pltpu.VMEM((sp, wr, cols), BF16),
            dma((nt,)), dma((nt,)), dma((sp - 1,)), dma((sp - 1,)), dma((nz,)), dma((nz,)),
            dma((nz - 1,)), dma((nz - 1,)), dma((nt,)), dma((nt,)),
        ],
        compiler_params=pltpu.CompilerParams(
            vmem_limit_bytes=62 * 1024 * 1024, collective_id=1, has_side_effects=True
        ),
        name="scatter",
    )(back_t, back_m, tok_all, w_all, dv)


def body(tokens, query_weight, key_weight, values, lambdas, out_grad):
    sp = lax.axis_size("sp")
    dp = lax.axis_size("dp")
    rows = tokens.shape[1]
    heads = lambdas.shape[0] // sp
    cos, sin = rotation_tables(rows * sp)
    tok_all, vog_all, w_all, qk = gather(
        tokens[0], values[0], out_grad[0], query_weight, key_weight, sp, dp
    )
    back_t, back_m, dv = attention(qk, vog_all, lambdas, cos, sin, heads)
    tokens_grad, values_grad, qg, kg = scatter(back_t, back_m, tok_all, w_all, dv, sp, dp)
    factor = 1.0 / math.sqrt(dp * rows * sp)
    return tokens_grad[None], values_grad[None], qg.astype(F32) * factor, kg.astype(F32) * factor


def solution(mesh):
    x = P("dp", "sp", None)
    w = P("dp", None)
    return jax.shard_map(
        body, mesh=mesh, in_specs=(x, w, w, x, P(), x), out_specs=(x, x, w, w), check_vma=False
    )
```
